32 devices in a mesh: fs: 4 (over z), tp: 8 (over y, x, core).
Axes of the slice: x: 2, y: 2, z: 4, core: 2. Of those that a mesh axis runs over, the one named last changes fastest.
Arguments:
- tokens: bfloat16 [1024, 2048], P('fs', 'tp'), may hold values from -6 to 6
- norm_gain: float32 [2048], P('tp'), may hold values from 0.1 to 1.9
- gate_master: float32 [8, 3584, 2048], P(None, 'fs', 'tp'), may hold values from -0.125 to 0.125
- up_master: float32 [8, 3584, 2048], P(None, 'fs', 'tp'), may hold values from -0.125 to 0.125
- down_master: float32 [8, 3584, 2048], P(None, 'fs', 'tp'), may hold values from -0.0625 to 0.0625
- routes: int32 [1024, 2], P('fs'), may hold values from 0 to 3, all different within a row; in each aligned block of 256 rows (0 to 255, 256 to 511, ...) at most 128 rows name the same one
- route_logits: float32 [1024, 2], P('fs'), may hold values from -8 to 8
Outputs:
- gate_serve: bfloat16 [8, 3584, 2048], P('tp', 'fs')
- up_serve: bfloat16 [8, 3584, 2048], P('tp', 'fs')
- down_serve: bfloat16 [8, 3584, 2048], P('tp', 'fs')
- mixed_tokens: bfloat16 [1024, 2048], P('fs', 'tp')
The draws below stay inside these ranges and needn't reach their ends.
Inputs may be any that keep to these rules, and one draw needn't show every extreme that they name: `routes`: each row names 2 different experts; in every aligned block of 256 rows each expert is named by exactly 128 rows.
All inputs are finite; a program needn't handle non-finite values.
Results may differ from the reference program's by a relative error of at most 0.024.
Values may be sent and summed in bfloat16 or wider, within the bound.
A program may use at most 128 MiB of HBM per device.

```python
import math
import jax
import jax.numpy as jnp
import numpy as np
from jax import lax

D = 2048
FF = 7168
TOP = 2
TOK_DEV = 256
EXPERTS = 4
SLABS = 8
FF_SLAB = 3584
TOKENS = 1024
CAP = 128
N_FS = 4


def block_levels(key, extent, pieces, low, top_value):
    def one(position, shards_of):
        steps = jax.random.uniform(jax.random.fold_in(jax.random.fold_in(key, 6), position), (shards_of,), jnp.float32, low / len(pieces), top_value / len(pieces))
        return jnp.repeat(jnp.exp(steps), extent[position] // shards_of).reshape((-1,) + (1,) * (len(extent) - position - 1))

    factor_of = one(*pieces[0])
    for cut in pieces[1:]:
        factor_of = factor_of * one(*cut)
    return factor_of


def assign_block(own_key, own, number, rows, number_of, top, bound, lean):
    order = jax.random.permutation(own_key, number_of)
    crowded, common = portions_of(number_of, rows * top, bound, lean, True), portions_of(number_of, rows * top, bound, lean, False)
    places = jnp.arange(number_of)

    def named(sizes, offset_by):
        used = int((sizes > 0).sum())
        fixed = max(1, used // 4)
        shifted = fixed + (places - fixed + offset_by * (used - fixed)) % max(1, number_of - fixed)
        return jnp.zeros((number_of,), jnp.int32).at[order[jnp.where(places < fixed, places, shifted)]].set(jnp.asarray(sizes, jnp.int32))

    sizes = jnp.where(number % 4 == 0, named(crowded, number // 4), named(common, number - number // 4 - 1))
    mixed = jax.random.permutation(jax.random.fold_in(own, 3), number_of)
    giver, sink = mixed[0:number_of // 2 * 2:2], mixed[1:number_of // 2 * 2:2]
    margin = jnp.minimum(sizes[giver] - 1, bound - sizes[sink]) // 2
    margin = jnp.where((giver == order[0]) | (sink == order[0]) | (sizes[sink] == 0), 0, jnp.maximum(margin, 0))
    shifted = jax.random.randint(jax.random.fold_in(own, 4), (number_of // 2,), 0, 1 << 20) % (margin + 1)
    sizes = sizes.at[giver].add(-shifted).at[sink].add(shifted)
    items = jnp.searchsorted(jnp.cumsum(sizes), jnp.arange(rows * top), side="right").astype(jnp.int32)
    grid = items.reshape(top, rows).T
    grid = grid[jax.random.permutation(jax.random.fold_in(own, 1), rows)]
    offset_by = jax.random.randint(jax.random.fold_in(own, 2), (rows, 1), 0, top)
    return jnp.take_along_axis(grid, (jnp.arange(top)[None, :] + offset_by) % top, axis=1)


def portions_of(number_of, total, limit, slope, full):
    weights = [(1 << 20) // math.isqrt(standing ** slope) + 1 for standing in range(1, number_of + 1)]
    largest = limit if full else min(limit, max(-(-total // number_of), total * weights[0] // sum(weights)))
    least = 1 if total - largest >= number_of - 1 else 0
    counts, spare = [largest] + [least] * (number_of - 1), total - largest - least * (number_of - 1)
    while spare > 0:
        candidates = [i for i in range(1, number_of) if counts[i] < largest] or [i for i in range(1, number_of) if counts[i] < limit]
        pool, left = sum([weights[i] for i in candidates]), spare
        for i in candidates:
            addition = min(limit - counts[i], max(1, left * weights[i] // pool), spare)
            counts[i] = counts[i] + addition
            spare = spare - addition
    return np.array(counts)


def normal_values(key, shape, width, limit, split=(), kind=jnp.bfloat16):
    drawn = width * jax.random.normal(key, shape, jnp.float32)
    if split:
        drawn = drawn * block_levels(key, shape, split, -0.22, 0.18)
    return jnp.clip(drawn, -limit, limit).astype(kind)


def setup_inputs(seed: int = 0) -> dict:
    seeds = jax.random.split(jax.random.key(seed), 8)
    tokens = normal_values(seeds[0], (TOKENS, D), 1.0, 6.0, ((0, 4), (1, 8)))
    norm_gain = jnp.clip(1.0 + 0.18 * jax.random.normal(seeds[1], (D,), jnp.float32), 0.1, 1.9)
    gate_master = normal_values(seeds[2], (SLABS, FF_SLAB, D), D ** -0.5, 0.125, ((1, 4), (2, 8)), jnp.float32)
    up_master = normal_values(seeds[3], (SLABS, FF_SLAB, D), D ** -0.5, 0.125, ((1, 4), (2, 8)), jnp.float32)
    down_master = normal_values(seeds[4], (SLABS, FF_SLAB, D), FF ** -0.5, 0.0625, ((1, 4), (2, 8)), jnp.float32)
    routes_keys = jax.random.split(jax.random.fold_in(seeds[5], 1), TOKENS // TOK_DEV)
    routes_turns = jax.random.permutation(jax.random.fold_in(seeds[5], 3), TOKENS // TOK_DEV)
    routes = jax.vmap(lambda own, number: assign_block(jax.random.fold_in(seeds[5], 2), own, number, TOK_DEV, EXPERTS, TOP, CAP, 0))(routes_keys, routes_turns).reshape((TOKENS, TOP))
    route_logits = normal_values(seeds[6], (TOKENS, TOP), 2.0, 8.0, ((0, 4),), jnp.float32)
    return dict(tokens=tokens, norm_gain=norm_gain, gate_master=gate_master, up_master=up_master, down_master=down_master, routes=routes, route_logits=route_logits)


epsilon = 1e-05

def reference(tokens, norm_gain, gate_master, up_master, down_master, routes, route_logits):
    gain_row = norm_gain[None, None, :]
    gate_serve = (gate_master * gain_row).astype(jnp.bfloat16)
    up_serve = (up_master * gain_row).astype(jnp.bfloat16)
    down_serve = down_master.astype(jnp.bfloat16)
    widened = tokens.astype(jnp.float32)
    row_scale = lax.rsqrt(lax.optimization_barrier(jnp.mean(widened * widened, axis=-1, keepdims=True)) + epsilon)
    normed = (widened * row_scale).astype(jnp.bfloat16)
    first_prob = jax.nn.sigmoid(route_logits[:, 0] - route_logits[:, 1])
    choice_prob = jnp.stack([first_prob, 1.0 - first_prob], axis=1)
    row_total = N_FS * CAP
    block_rows = FF_SLAB // N_FS

    def one_expert(expert_id):
        matches = routes == expert_id
        is_member = jnp.any(matches, axis=1)
        weight = lax.optimization_barrier(jnp.sum(jnp.where(matches, choice_prob, 0.0), axis=1))
        row_index = jnp.nonzero(is_member, size=row_total)[0].astype(jnp.int32)
        picked = normed[row_index]
        block_parts = jnp.zeros((N_FS, row_total, D), jnp.float32)
        for half_index in range(2):
            slab_id = 2 * expert_id + half_index
            gate_slab = lax.dynamic_index_in_dim(gate_serve, slab_id, 0, keepdims=False)
            up_slab = lax.dynamic_index_in_dim(up_serve, slab_id, 0, keepdims=False)
            down_slab = lax.dynamic_index_in_dim(down_serve, slab_id, 0, keepdims=False)
            gate_pre = jnp.dot(picked, gate_slab.T, preferred_element_type=jnp.float32)
            up_pre = jnp.dot(picked, up_slab.T, preferred_element_type=jnp.float32)
            hidden = (jax.nn.silu(gate_pre) * up_pre).astype(jnp.bfloat16)
            block_parts = block_parts + jnp.einsum('rfk,fkd->frd', hidden.reshape(row_total, N_FS, block_rows).astype(jnp.float32), down_slab.reshape(N_FS, block_rows, D).astype(jnp.float32))
        rounded = lax.optimization_barrier(block_parts.astype(jnp.bfloat16))
        expert_out = lax.optimization_barrier(jnp.sum(rounded.astype(jnp.float32), axis=0)).astype(jnp.bfloat16)
        return (row_index, weight[row_index][:, None] * expert_out.astype(jnp.float32))
    expert_ids = jnp.arange(EXPERTS, dtype=jnp.int32)
    all_index, all_terms = lax.map(one_expert, expert_ids)
    mixed = jnp.zeros((TOKENS, D), jnp.float32).at[all_index.reshape(-1)].add(all_terms.reshape(-1, D))
    return (gate_serve, up_serve, down_serve, mixed.astype(jnp.bfloat16))
```

```python
import functools

import jax
import jax.numpy as jnp
from jax import lax
from jax.experimental import pallas as pl
from jax.experimental.pallas import tpu as pltpu
from jax.sharding import PartitionSpec as P

epsilon = 1e-05
MESH = pl.DeviceIdType.MESH
NT = (((1,), (1,)), ((), ()))
NN = (((1,), (0,)), ((), ()))
TN = (((0,), (0,)), ((), ()))
SLOTS = 4


def dot(a, b, dims):
    return lax.dot_general(a, b, dims, preferred_element_type=jnp.float32)


def flipped(index, mask):
    result, bit = index, 1
    while bit <= mask:
        if mask & bit:
            result = result + bit * (1 - 2 * ((index // bit) % 2))
        bit *= 2
    return result


def kernel(
    nf, nt, tok_ref, gain_ref, gate_ref, up_ref, down_ref, routes_ref, logits_ref,
    gate_out, up_out, down_out, mixed_ref,
    stage, snd, wv, place, comb_hi, comb_lo, pick, xin, xall, gate_pre, hid, part, pin, psum, zin, ret,
    stage_sem, w_send, w_recv, x_send, x_recv, z_send, z_recv, p_send, p_recv,
    h_send, h_recv, s_send, s_recv, r_send, r_recv, out_sem,
):
    f, me = lax.axis_index("fs"), lax.axis_index("tp")
    parity = me % 2
    partner = me + 1 - 2 * parity
    rows, cols = tok_ref.shape
    block = gate_ref.shape[1]
    half = pick.shape[1]
    cap = 2 * half
    experts = nt // 2
    masters = (gate_ref, up_ref, down_ref)
    outs = (gate_out, up_out, down_out)
    order = list(range(nt - 1, -1, -1))
    jobs = [(w, k) for w in range(3) for k in order]

    def load(i):
        w, k = jobs[i]
        return pltpu.make_async_copy(
            masters[w].at[flipped(me, k)], stage.at[i % SLOTS], stage_sem.at[i % SLOTS]
        )

    def remote(src, dst, send, recv, to_f, to_t):
        return pltpu.make_async_remote_copy(
            src_ref=src, dst_ref=dst, send_sem=send, recv_sem=recv,
            device_id=(to_f, to_t), device_id_type=MESH,
        )

    for i in range(SLOTS):
        load(i).start()
    barrier = pltpu.get_barrier_semaphore()
    for k in range(1, nt):
        pl.semaphore_signal(barrier, inc=1, device_id=(f, flipped(me, k)), device_id_type=MESH)

    @pl.loop(1, nf)
    def _(d):
        pl.semaphore_signal(barrier, inc=1, device_id=((f + d) % nf, me), device_id_type=MESH)

    pl.semaphore_wait(barrier, nt - 1 + nf - 1)

    step = 128 if block % 128 == 0 else block

    def weight_copy(w, k):
        return remote(
            snd.at[w, k - 1], wv.at[w, me], w_send.at[w, k - 1], w_recv.at[w, k - 1], f, flipped(me, k)
        )

    def convert(i):
        w, k = jobs[i]
        slot = i % SLOTS
        load(i).wait()
        gain = gain_ref[...]

        @pl.loop(0, block // step)
        def _(c):
            at = pl.ds(pl.multiple_of(c * step, 16), step)
            value = stage[slot, at, :]
            if w < 2:
                value = value * gain
            value = value.astype(jnp.bfloat16)
            if k:
                snd[w, k - 1, at, :] = value
            else:
                wv[w, me, at, :] = value

        if k:
            weight_copy(w, k).start()
        if i + SLOTS < len(jobs):
            load(i + SLOTS).start()

    def x_copy(k):
        to = flipped(me, k)
        return remote(pick.at[to], xin.at[me], x_send.at[k - 1], x_recv.at[k - 1], f, to)

    def route():
        r0, r1 = routes_ref[0:1, :], routes_ref[1:2, :]
        l0, l1 = logits_ref[0:1, :], logits_ref[1:2, :]
        p0 = 1.0 / (1.0 + jnp.exp(l1 - l0))
        p1 = 1.0 / (1.0 + jnp.exp(l0 - l1))
        padded = -(-experts // 8) * 8
        ids = lax.broadcasted_iota(jnp.int32, (padded, rows), 0)
        first = jnp.where(ids == r0, 1.0, 0.0)
        second = jnp.where(ids == r1, 1.0, 0.0)
        chosen = first + second
        weight = first * p0 + second * p1
        before = lax.broadcasted_iota(jnp.int32, (rows, rows), 0)
        after = lax.broadcasted_iota(jnp.int32, (rows, rows), 1)
        upto = jnp.where(before <= after, 1.0, 0.0).astype(jnp.bfloat16)
        position = dot(chosen.astype(jnp.bfloat16), upto, NN) - 1.0
        slots = lax.broadcasted_iota(jnp.int32, (cap, rows), 0).astype(jnp.float32)
        for e in range(experts):
            hit = jnp.where(slots == position[e : e + 1, :], 1.0, 0.0) * chosen[e : e + 1, :]
            placed = hit.astype(jnp.bfloat16)
            scaled = hit * weight[e : e + 1, :]
            high = scaled.astype(jnp.bfloat16)
            at = pl.ds(e * cap, cap)
            comb_hi[at, :] = high
            comb_lo[at, :] = (scaled - high.astype(jnp.float32)).astype(jnp.bfloat16)
            got = dot(placed, tok_ref[...], NN).astype(jnp.bfloat16)
            pick[2 * e] = got[:half]
            pick[2 * e + 1] = got[half:]
        xin[me] = pick[me]
        for k in order[:-1]:
            x_copy(k).start()

    early = 2
    for i in range(early):
        convert(i)
    route()
    for i in range(early, len(jobs)):
        convert(i)

    for k in order[:-1]:
        x_copy(k).wait_recv()
    total = jnp.zeros((half, 1), jnp.float32)
    for s in range(nt):
        v = xin[s].astype(jnp.float32)
        total = total + jnp.sum(v * v, axis=-1, keepdims=True)
    scale = lax.rsqrt(total / (nt * cols) + epsilon)

    def rows_of(p, g):
        return pl.ds(pl.multiple_of((p * nf + g) * half, 16), half)

    mine = rows_of(parity, f)
    for s in range(nt):
        xall[s, mine, :] = (xin[s].astype(jnp.float32) * scale).astype(jnp.bfloat16)

    def z_copy(d):
        here = xall.at[:, mine, :]
        return remote(here, here, z_send.at[d], z_recv.at[d], (f + d) % nf, me)

    def p_copy(d):
        here = xall.at[:, rows_of(parity, (f + nf - d) % nf), :]
        return remote(here, here, p_send.at[d], p_recv.at[d], f, partner)

    p_copy(0).start()

    @pl.loop(1, nf)
    def _(d):
        z_copy(d).start()

    @pl.loop(1, nf)
    def _(d):
        here = xall.at[:, rows_of(parity, (f + nf - d) % nf), :]
        remote(here, here, z_send.at[d], z_recv.at[d], (f + d) % nf, me).wait_recv()
        p_copy(d).start()

    @pl.loop(0, nf)
    def _(d):
        here = xall.at[:, rows_of(1 - parity, (f + nf - d) % nf), :]
        remote(here, here, p_send.at[d], p_recv.at[d], f, partner).wait_recv()

    def out_copy(w, k):
        s = flipped(me, k)
        to = outs[w].at[0, :, pl.ds(pl.multiple_of(s * cols, 128), cols)]
        return pltpu.make_async_copy(wv.at[w, s], to, out_sem.at[w, k])

    def arrived(w, k):
        if k:
            s = flipped(me, k)
            remote(
                snd.at[w, k - 1], wv.at[w, s], w_send.at[w, k - 1], w_recv.at[w, k - 1], f, s
            ).wait_recv()
        out_copy(w, k).start()

    def product(w, at):
        acc = dot(xall[0], wv[w, 0, at, :], NT)
        for s in range(1, nt):
            acc = acc + dot(xall[s], wv[w, s, at, :], NT)
        return acc

    def tile(c):
        return pl.ds(pl.multiple_of(c * step, 16), step)

    def lanes(c):
        return pl.ds(pl.multiple_of(c * step, 128), step) if block % 128 == 0 else slice(None)

    for k in order:
        arrived(0, k)

    @pl.loop(0, block // step)
    def _(c):
        gate_pre[:, lanes(c)] = product(0, tile(c))

    for k in order:
        arrived(1, k)

    @pl.loop(0, block // step)
    def _(c):
        gate = gate_pre[:, lanes(c)]
        hid[:, lanes(c)] = (gate / (1.0 + jnp.exp(-gate)) * product(1, tile(c))).astype(jnp.bfloat16)

    side = nf * half

    def pair_at(g):
        return flipped(me // 2, nt // 2 - 1 - g)

    def side_rows(p):
        return pl.ds(pl.multiple_of(p * side, 16), side)

    def h_copy(g):
        q = pair_at(g)
        return remote(
            part.at[q, :, side_rows(1 - parity), :], pin.at[q], h_send.at[g], h_recv.at[g], f, partner
        )

    def s_copy(g, d):
        q, to = pair_at(g), (f + d) % nf
        return remote(psum.at[q, to], zin.at[g, d], s_send.at[g, d], s_recv.at[g, d], to, me)

    def r_copy(k):
        s = flipped(me, k)
        return remote(
            psum.at[s // 2, f, s % 2], ret.at[pl.ds(pl.multiple_of(me * half, 16), half), :],
            r_send.at[k - 1], r_recv.at[k - 1], f, s,
        )

    def stage_a(g):
        ks = (nt - 1 - 2 * g, nt - 2 - 2 * g)
        for k in ks:
            arrived(2, k)
        q = pair_at(g)
        for o in range(2):
            part[q, o] = dot(hid[...], wv[2, 2 * q + o], NN).astype(jnp.bfloat16)
        h_copy(g).start()

    def stage_b(g):
        q = pair_at(g)
        h_copy(g).wait_recv()
        for o in range(2):
            both = part[q, o, side_rows(parity), :].astype(jnp.float32) + pin[q, o].astype(jnp.float32)
            both = both.astype(jnp.bfloat16)
            for j in range(nf):
                psum[q, j, o] = both[j * half : (j + 1) * half]

        @pl.loop(1, nf)
        def _(d):
            s_copy(g, d).start()

    def stage_c(g):
        q = pair_at(g)

        @pl.loop(1, nf)
        def _(d):
            s_copy(g, d).wait_recv()

        for o in range(2):
            acc = psum[q, f, o].astype(jnp.float32)
            for d in range(1, nf):
                acc = acc + zin[g, d, o].astype(jnp.float32)
            psum[q, f, o] = acc.astype(jnp.bfloat16)
        for k in (nt - 1 - 2 * g, nt - 2 - 2 * g):
            if k:
                r_copy(k).start()
            else:
                ret[pl.ds(pl.multiple_of(me * half, 16), half), :] = psum[me // 2, f, me % 2]

    pairs = nt // 2
    for g in range(pairs):
        stage_a(g)
        stage_b(g)
        if g:
            stage_c(g - 1)
    stage_c(pairs - 1)
    for k in order[:-1]:
        r_copy(k).wait_recv()
    mixed = dot(comb_hi[...], ret[...], TN) + dot(comb_lo[...], ret[...], TN)
    mixed_ref[...] = mixed.astype(jnp.bfloat16)

    for k in order:
        for w in range(3):
            out_copy(w, k).wait()
            if k:
                weight_copy(w, k).wait_send()
        if k:
            x_copy(k).wait_send()
            r_copy(k).wait_send()
    p_copy(0).wait_send()

    @pl.loop(1, nf)
    def _(d):
        z_copy(d).wait_send()
        p_copy(d).wait_send()
        for g in range(pairs):
            s_copy(g, d).wait_send()

    for g in range(pairs):
        h_copy(g).wait_send()


def local(tokens, norm_gain, gate_master, up_master, down_master, routes, route_logits):
    nf, nt = lax.axis_size("fs"), lax.axis_size("tp")
    rows, cols = tokens.shape
    block = gate_master.shape[1]
    half = rows * routes.shape[1] // nt
    every = 2 * nf * half
    pairs = nt // 2
    bf16 = jnp.bfloat16
    served = jax.ShapeDtypeStruct((1, block, nt * cols), bf16)
    hbm = pl.BlockSpec(memory_space=pl.ANY)
    vmem = pl.BlockSpec(memory_space=pltpu.VMEM)
    dma = pltpu.SemaphoreType.DMA
    return pl.pallas_call(
        functools.partial(kernel, nf, nt),
        out_shape=(served, served, served, jax.ShapeDtypeStruct((rows, cols), bf16)),
        in_specs=[vmem, vmem, hbm, hbm, hbm, vmem, vmem],
        out_specs=(hbm, hbm, hbm, vmem),
        scratch_shapes=[
            pltpu.VMEM((SLOTS, block, cols), jnp.float32),
            pltpu.VMEM((3, nt - 1, block, cols), bf16),
            pltpu.VMEM((3, nt, block, cols), bf16),
            pltpu.VMEM((16, 128), bf16),
            pltpu.VMEM((nt * half, rows), bf16),
            pltpu.VMEM((nt * half, rows), bf16),
            pltpu.VMEM((nt, half, cols), bf16),
            pltpu.VMEM((nt, half, cols), bf16),
            pltpu.VMEM((nt, every, cols), bf16),
            pltpu.VMEM((every, block), jnp.float32),
            pltpu.VMEM((every, block), bf16),
            pltpu.VMEM((pairs, 2, every, cols), bf16),
            pltpu.VMEM((pairs, 2, every // 2, cols), bf16),
            pltpu.VMEM((pairs, nf, 2, half, cols), bf16),
            pltpu.VMEM((pairs, nf, 2, half, cols), bf16),
            pltpu.VMEM((nt * half, cols), bf16),
            dma((SLOTS,)),
            dma((3, nt - 1)), dma((3, nt - 1)),
            dma((nt - 1,)), dma((nt - 1,)),
            dma((nf,)), dma((nf,)),
            dma((nf,)), dma((nf,)),
            dma((pairs,)), dma((pairs,)),
            dma((pairs, nf)), dma((pairs, nf)),
            dma((nt - 1,)), dma((nt - 1,)),
            dma((3, nt)),
        ],
        compiler_params=pltpu.CompilerParams(
            collective_id=0, has_side_effects=True, vmem_limit_bytes=62 * 1024 * 1024
        ),
    )(tokens, norm_gain.reshape(1, cols), gate_master, up_master, down_master, routes.T, route_logits.T)


def solution(mesh):
    placed = (
        P("fs", "tp"),
        P("tp"),
        P(None, "fs", "tp"),
        P(None, "fs", "tp"),
        P(None, "fs", "tp"),
        P("fs", None),
        P("fs", None),
    )
    return jax.shard_map(
        local,
        mesh=mesh,
        in_specs=placed,
        out_specs=(P("tp", "fs", None), P("tp", "fs", None), P("tp", "fs", None), P("fs", "tp")),
        check_vma=False,
    )
```
